32 devices in a mesh: grp: 2 (over y), fs: 4 (over z), tp: 4 (over x, core).
Axes of the slice: x: 2, y: 2, z: 4, core: 2. Of those that a mesh axis runs over, the one named last changes fastest.
Arguments:
- prompt_rows: bfloat16 [8192, 2048], P(('grp', 'fs')), parts along dimension 0, may hold values from -6 to 6
- up_master: float32 [2048, 8192], P('fs', 'tp'), may hold values from -0.125 to 0.125
- down_master: float32 [8192, 2048], P('fs', 'tp'), may hold values from -0.0625 to 0.0625
- norm_gain: float32 [2048], P('fs'), may hold values from 0.1 to 1.9
Outputs:
- up_sampler: bfloat16 [8, 2048, 2048], P(('grp', 'tp')), parts along dimension 0
- down_sampler: bfloat16 [8, 2048, 2048], P(('grp', 'tp')), parts along dimension 0
- layer_out: bfloat16 [8192, 2048], P(('grp', 'fs', 'tp')), parts along dimension 0
The draws below stay inside these ranges and needn't reach their ends.
There are 2 independent parts, one for each index of `grp`. The reference program is written for one: setup_inputs(seed, part) draws one part's arguments, and reference() takes and returns one part's arrays. A program takes and returns all parts, laid end to end along the dimension named above; an argument that names none is the same for every part. Nothing has to cross between parts.
All inputs are finite; a program needn't handle non-finite values.
Results may differ from the reference program's by a relative error of at most 0.014.
Values may be sent and summed in bfloat16 or wider, within the bound.
A program may use at most 128 MiB of HBM per device.

```python
import jax
import jax.numpy as jnp
from jax import lax

D = 2048
FF = 8192
TOKENS = 4096
UNIT_SPAN = 512
N_FS = 4
N_TP = 4


def block_scale(rng, extent, split, low, largest):
    level, own = 1.0, jax.random.fold_in(rng, 6)
    for dim, blocks in split:
        steps = jnp.exp(jax.random.uniform(jax.random.fold_in(own, dim), (blocks,), jnp.float32, low / len(split), largest / len(split)))
        level = level * jnp.repeat(steps, extent[dim] // blocks).reshape([-1 if axis == dim else 1 for axis in range(len(extent))])
    return level


def noise(stream_key, shape, width, reach, cuts=(), kind=jnp.bfloat16):
    gain = block_scale(stream_key, shape, cuts, -0.22, 0.18) if cuts else 1.0
    drawn = jax.random.normal(stream_key, shape, jnp.float32) * width * gain
    return jnp.minimum(jnp.maximum(drawn, -reach), reach).astype(kind)


def setup_inputs(seed: int = 0, part: int = 0) -> dict:
    key_of = jax.random.split(jax.random.key(seed), 5)
    part_splits = jax.random.split(jax.random.fold_in(key_of[4], part), 5)
    prompt_rows = noise(part_splits[0], (TOKENS, D), 1.0, 6.0, ((0, 4),))
    up_master = noise(key_of[1], (D, FF), D ** -0.5, 0.125, ((0, 4), (1, 4)), jnp.float32)
    down_master = noise(key_of[2], (FF, D), FF ** -0.5, 0.0625, ((0, 4), (1, 4)), jnp.float32)
    norm_gain = jnp.clip(1.0 + 0.18 * jax.random.normal(key_of[3], (D,), jnp.float32), 0.1, 1.9)
    return {"prompt_rows": prompt_rows, "up_master": up_master, "down_master": down_master, "norm_gain": norm_gain}


eps = 1e-06

def reference(prompt_rows, up_master, down_master, norm_gain):
    folded = (up_master * norm_gain[:, None]).astype(jnp.bfloat16)
    down_cast = down_master.astype(jnp.bfloat16)
    up_sampler = folded.reshape(D, N_FS, N_TP, UNIT_SPAN).transpose(2, 0, 1, 3).reshape(N_TP, D, N_FS * UNIT_SPAN)
    down_sampler = down_cast.reshape(N_FS, N_TP, UNIT_SPAN, D).transpose(1, 0, 2, 3).reshape(N_TP, N_FS * UNIT_SPAN, D)
    values = prompt_rows.astype(jnp.float32)
    normed = (values * lax.rsqrt(lax.optimization_barrier(jnp.mean(values * values, axis=-1, keepdims=True)) + eps)).astype(jnp.bfloat16)
    total = jnp.zeros((prompt_rows.shape[0], D), jnp.float32)
    for group in range(N_TP):
        pre_act = jnp.dot(normed, up_sampler[group], preferred_element_type=jnp.float32)
        hidden = jnp.square(jax.nn.relu(pre_act)).astype(jnp.bfloat16)
        partial_value = jnp.dot(hidden, down_sampler[group], preferred_element_type=jnp.float32).astype(jnp.bfloat16)
        partial_value = lax.optimization_barrier(partial_value)
        total = total + partial_value.astype(jnp.float32)
    return (up_sampler, down_sampler, total.astype(jnp.bfloat16))
```

```python
import functools
import math

import jax
import jax.numpy as jnp
from jax import lax
from jax.experimental import pallas as pl
from jax.experimental.pallas import tpu as pltpu
from jax.sharding import PartitionSpec as P

eps = 1e-06
row_tile = 256
norm_tile = 64
pieces = 2
MESH = pl.DeviceIdType.MESH


def column_groups(tp, widths):
    groups = []
    for w in range(2):
        for j in range(tp):
            width = 256 if widths[w] % 256 == 0 else widths[w]
            if w == 1 and j == tp - 1 and width == 256:
                width = 128
            for first in range(0, widths[w], width):
                groups.append((w, j, first, width))
    return groups


def own_plan(count, steps, ahead, behind):
    plan, sent = [], ahead
    early, late = count * 2 // 9, count * 2 // 3
    for step in range(steps):
        if step < early:
            lead = ahead
        elif step >= late:
            lead = behind
        else:
            lead = round(ahead + (behind - ahead) * (step - early + 1) / (late - early + 1))
        now = []
        while sent < count and (sent <= step + lead or step == steps - 1):
            now.append(sent)
            sent += 1
        plan.append(now)
    return plan


def gather_kernel(
    n, tp, groups, up_ref, down_ref, gain_ref, rows_ref, up_all, down_all, part, arrived,
    normed, hidden, total, up_stage, down_stage, up_cast, down_cast, gain_tall, load_sem,
    tp_send, tp_recv, z_send, z_recv, y_send, y_recv, sum_send, sum_recv,
):
    y = lax.axis_index("grp")
    z = lax.axis_index("fs")
    me = lax.axis_index("tp")
    chips = tp // 2
    depths = (up_ref.shape[0], down_ref.shape[0] // tp)
    widths = (up_ref.shape[1] // tp, down_ref.shape[1])
    alls = (up_all, down_all)
    tokens = rows_ref.shape[0]
    share = tokens // tp
    count = len(groups)
    first_down = sum(group[0] == 0 for group in groups)
    twins = n > 2
    lag = max(n - 2, 2)
    steps = count + lag
    ahead, lead = 2, 3
    plan = own_plan(count, steps, ahead, -1)
    middle = jnp.logical_and(z > 0, z < n - 1)

    def source(device, j):
        return lax.rem(device // 2 + j // 2, chips) * 2 + lax.rem(lax.rem(device, 2) + j % 2, 2)

    def target(j):
        return lax.rem(me // 2 + chips - j // 2, chips) * 2 + lax.rem(lax.rem(me, 2) + j % 2, 2)

    far_first = [k for k in range(2, tp)] + [1]

    def columns(g, b):
        w, _, first, width = groups[g]
        return pl.ds(pl.multiple_of(b * widths[w] + first, math.gcd(width, 256)), width)

    def rows(w, a, h):
        half = depths[w] // 2
        return pl.ds(pl.multiple_of(a * depths[w] + h * half, half), half)

    def block(g, a, h):
        w, j, _, _ = groups[g]
        return alls[w].at[rows(w, a, h), columns(g, source(me, j))]

    def wide(w, b):
        return pl.ds(pl.multiple_of(b * widths[w], widths[w]), widths[w])

    def remote(src, dst, send, recv, device):
        return pltpu.make_async_remote_copy(
            src_ref=src, dst_ref=dst, send_sem=send, recv_sem=recv,
            device_id=device, device_id_type=MESH,
        )

    def half_of(k):
        return y if k == 0 else 1 - y

    def tp_copy(w, j, k):
        half = depths[w] // 2
        t = target(j)
        if w == 0:
            src = up_cast.at[pl.ds(pl.multiple_of(half_of(k) * half, half), half), wide(0, t)]
        else:
            src = down_cast.at[pl.ds(pl.multiple_of(t * depths[1] + half_of(k) * half, half), half), :]
        dst = alls[w].at[rows(w, z, half_of(k)), wide(w, me)]
        return remote(src, dst, tp_send.at[w], tp_recv.at[w, j - 1, k], {"tp": t})

    def tp_arrival(w, j, k):
        ref = alls[w].at[rows(w, z, half_of(k)), wide(w, source(me, j))]
        return remote(ref, ref, tp_send.at[w], tp_recv.at[w, j - 1, k], {"tp": target(j)})

    def in_pieces(g):
        return groups[g][0] == 1 and g >= count - pieces and depths[1] % 128 == 0

    def half_sem(g, a):
        return y_recv.at[count + (g - count + pieces) * n + a if in_pieces(g) else g]

    def z_copy(g, a, way, device):
        ref = block(g, a, y)
        slot = lax.rem(a - device + n, n) - 1
        return remote(ref, ref, z_send.at[way], z_recv.at[g, slot], {"fs": device})

    def own_up(g):
        return z_copy(g, z, 0, z + 1)

    def own_down(g):
        return z_copy(g, z, 1, z - 1)

    def twin_copy(g, a, device):
        ref = block(g, a, 1 - y)
        return remote(ref, ref, z_send.at[2], half_sem(g, a), {"fs": device})

    def y_copy(g, a, h):
        ref = block(g, a, h)
        return remote(ref, ref, y_send.at[0], half_sem(g, a), {"grp": 1 - y})

    def sum_copy(g, k):
        t = target(k)
        cols = columns(g, source(me, groups[g][1]))
        src = part.at[pl.ds(pl.multiple_of(t * share, share), share), cols]
        return remote(src, arrived.at[k - 1, :, cols], sum_send.at[0], sum_recv.at[0], {"tp": t})

    def up_load(j):
        half = depths[0] // 2
        here = pl.ds(pl.multiple_of(y * half, half), half)
        cols = wide(0, target(j))
        return pltpu.make_async_copy(up_ref.at[here, cols], up_stage.at[here, cols], load_sem.at[j])

    def late_load():
        half = depths[0] // 2
        here = pl.ds(pl.multiple_of((1 - y) * half, half), half)
        return pltpu.make_async_copy(up_ref.at[here, :], up_stage.at[here, :], load_sem.at[tp])

    down_load = pltpu.make_async_copy(down_ref, down_stage, load_sem.at[tp + 1])
    rows_load = pltpu.make_async_copy(rows_ref, normed, load_sem.at[tp + 2])
    order = [0] + far_first
    for j in order:
        up_load(j).start()
    late_load().start()
    rows_load.start()
    down_load.start()
    barrier = pltpu.get_barrier_semaphore()
    for j in range(1, tp):
        pl.semaphore_signal(barrier, inc=1, device_id={"tp": target(j)}, device_id_type=MESH)
    pl.semaphore_signal(barrier, inc=1, device_id={"grp": 1 - y}, device_id_type=MESH)

    @pl.when(z > 0)
    def _():
        pl.semaphore_signal(barrier, inc=1, device_id={"fs": z - 1}, device_id_type=MESH)

    @pl.when(z < n - 1)
    def _():
        pl.semaphore_signal(barrier, inc=1, device_id={"fs": z + 1}, device_id_type=MESH)

    gain_tall[...] = jnp.broadcast_to(gain_ref[...], (128, depths[0])).T

    def cast_up(j, k):
        half = depths[0] // 2
        tile = math.gcd(half, norm_tile)
        cols = wide(0, target(j))

        @pl.loop(0, half // tile)
        def _(m):
            first = pl.multiple_of(half_of(k) * half + m * tile, tile)
            here = pl.ds(first, tile)
            value = (up_stage[here, cols] * gain_tall[here, :1]).astype(jnp.bfloat16)
            if j == 0:
                up_all[pl.ds(pl.multiple_of(z * depths[0] + first, tile), tile), cols] = value
            else:
                up_cast[here, cols] = value

    def cast_down():
        tile = math.gcd(depths[1], norm_tile)

        @pl.loop(0, down_ref.shape[0] // tile)
        def _(m):
            here = pl.ds(pl.multiple_of(m * tile, tile), tile)
            down_cast[here, :] = down_stage[here, :].astype(jnp.bfloat16)

        @pl.loop(0, depths[1] // tile)
        def _(m):
            here = pl.ds(pl.multiple_of(me * depths[1] + m * tile, tile), tile)
            there = pl.ds(pl.multiple_of(z * depths[1] + m * tile, tile), tile)
            down_all[there, wide(1, me)] = down_stage[here, :].astype(jnp.bfloat16)

    def norm_rows(first, many):
        @pl.loop(0, many // norm_tile)
        def _(m):
            here = pl.ds(pl.multiple_of(first + m * norm_tile, norm_tile), norm_tile)
            values = normed[here, :].astype(jnp.float32)
            scale = lax.rsqrt(jnp.mean(values * values, axis=-1, keepdims=True) + eps)
            normed[here, :] = (values * scale).astype(jnp.bfloat16)

    def late_own(g):
        @pl.when(z == 1)
        def _():
            own_down(g).start()

        @pl.when(z == n - 2)
        def _():
            own_up(g).start()

    def early_own(g):
        w, j, first, _ = groups[g]
        if j > 0 and first == 0:
            tp_arrival(w, j, 0).wait_recv()

        @pl.when(z > 1)
        def _():
            own_down(g).start()

        @pl.when(z < n - 2)
        def _():
            own_up(g).start()

    def twin_own(g):
        w, j, first, _ = groups[g]
        if j > 0 and first == 0:
            tp_arrival(w, j, 1).wait_recv()
        if twins:
            for edge, near in ((0, 1), (n - 1, n - 2)):

                @pl.when(z == edge)
                def _():
                    twin_copy(g, edge, near).start()

    def at_edge(body):
        for edge, way in ((0, 1), (n - 1, -1)):

            @pl.when(z == edge)
            def _():
                body(lambda s: edge + way * s)

    def edge_receive(g, a):
        z_copy(g, a, 0, z).wait_recv()
        y_copy(g, a, y).start()

    def receive(step):
        @pl.when(middle)
        def _():
            for s in range(1, n - 1):
                g = step - (s - 1)
                if not 0 <= g < count:
                    continue

                @pl.when(z >= s)
                def _():
                    a = z - s
                    z_copy(g, a, 0, z).wait_recv()
                    z_copy(g, a, 0, z + 1).start()
                    if s == 1 and twins:

                        @pl.when(a != 0)
                        def _():
                            y_copy(g, a, y).start()
                    else:
                        y_copy(g, a, y).start()

                @pl.when(z + s < n)
                def _():
                    a = z + s
                    z_copy(g, a, 0, z).wait_recv()
                    z_copy(g, a, 1, z - 1).start()
                    if s == 1 and twins:

                        @pl.when(a != n - 1)
                        def _():
                            y_copy(g, a, y).start()
                    else:
                        y_copy(g, a, y).start()

        def edge(at):
            for s in range(2, n):
                g = step - (s - 2)
                if 0 <= g < count:
                    edge_receive(g, at(s))
            for g in plan[step]:
                edge_receive(g, at(1))

        at_edge(edge)

    def other_half(g, a):
        y_copy(g, a, 1 - y).wait_recv()

    def other_halves(g):
        w = groups[g][0]
        half = depths[w] // 2
        ref = alls[w].at[pl.ds(0, (n - 1) * half), columns(g, source(me, groups[g][1]))]
        remote(ref, ref, y_send.at[0], y_recv.at[g], {"grp": 1 - y}).wait_recv()

    def finish(g):
        w, j, _, width = groups[g]
        cols = columns(g, source(me, j))

        def product(a, fresh):
            deep = pl.ds(pl.multiple_of(a * depths[1], depths[1]), depths[1])

            @pl.loop(0, tokens // row_tile)
            def _(m):
                here = pl.ds(pl.multiple_of(m * row_tile, row_tile), row_tile)
                acc = jnp.dot(hidden[here, deep], down_all[deep, cols], preferred_element_type=jnp.float32)
                total[here, :] = acc if fresh else total[here, :] + acc

        if in_pieces(g):
            product(z, True)
            for s in range(1, n):
                for a in range(n):
                    if a - s < 0 and a + s > n - 1:
                        continue
                    near = z - a == s if a + s < n else a - z == s
                    if a + s < n and a - s >= 0:
                        near = jnp.logical_or(z - a == s, a - z == s)

                    @pl.when(near)
                    def _():
                        other_half(g, a)
                        product(a, False)

            @pl.loop(0, tokens // row_tile)
            def _(m):
                here = pl.ds(pl.multiple_of(m * row_tile, row_tile), row_tile)
                part[here, cols] = total[here, :].astype(jnp.bfloat16)
        else:
            other_halves(g)

            @pl.loop(0, tokens // row_tile)
            def _(m):
                here = pl.ds(pl.multiple_of(m * row_tile, row_tile), row_tile)
                if w == 0:
                    acc = jnp.dot(normed[here, :], up_all[:, cols], preferred_element_type=jnp.float32)
                    acc = jnp.maximum(acc, 0.0)
                    hidden[here, cols] = (acc * acc).astype(jnp.bfloat16)
                else:
                    acc = jnp.dot(hidden[here, :], down_all[:, cols], preferred_element_type=jnp.float32)
                    part[here, cols] = acc.astype(jnp.bfloat16)

        if w == 1:
            for k in far_first:
                sum_copy(g, k).start()

    up_load(0).wait()
    cast_up(0, 0)
    pl.semaphore_wait(barrier, tp + (z + n - 1) // n + (2 * n - 2 - z) // n)
    for g in range(ahead):
        early_own(g)
        late_own(g)
    for j in far_first:
        up_load(j).wait()
        cast_up(j, 0)
        tp_copy(0, j, 0).start()
    late_load().wait()
    for j in far_first + [0]:
        cast_up(j, 1)
        if j > 0:
            tp_copy(0, j, 1).start()
    rows_load.wait()
    quarter = tokens // 4

    def down_work():
        down_load.wait()
        cast_down()
        for k in range(2):
            for j in far_first:
                tp_copy(1, j, k).start()

    work = [functools.partial(norm_rows, i * quarter, quarter) for i in range(4)] + [down_work]
    for g in range(ahead):
        at_edge(lambda at: edge_receive(g, at(1)))
        work.pop(0)()
    sent = ahead
    for step in range(steps):
        receive(step)
        while sent < count and sent <= step + lead:
            early_own(sent)
            sent += 1
        for g in plan[step]:
            late_own(g)
        if step < count:
            twin_own(step)
        if work:
            work.pop(0)()
        if step >= lag:
            while work:
                work.pop(0)()
            finish(step - lag)

    def await_sends(ref, sem):
        remote(ref, ref, sem, sum_recv.at[0], {"grp": 1 - y}).wait_send()

    await_sends(up_cast.at[:, pl.ds(0, (tp - 1) * widths[0])], tp_send.at[0])
    await_sends(down_cast.at[pl.ds(0, (tp - 1) * depths[1]), :], tp_send.at[1])
    for edge in range(n):
        passed = n - 1 - (twins and edge == 1) - (twins and edge == n - 2)
        waits = [
            (z_send.at[0], edge + 1 if edge < n - 1 else 0),
            (z_send.at[1], n - edge if edge > 0 else 0),
            (z_send.at[2], int(twins and edge in (0, n - 1))),
            (y_send.at[0], passed),
        ]

        @pl.when(z == edge)
        def _():
            for sem, blocks in waits:
                if blocks:
                    await_sends(up_all.at[pl.ds(0, blocks * depths[0]), :], sem)

    remote(arrived, arrived, sum_send.at[0], sum_recv.at[0], {"grp": 1 - y}).wait()


def place_kernel(tp, up_in, down_in, part, arrived, up_out, down_out, layer_out, layer, sem):
    share = layer.shape[0]
    me = lax.axis_index("tp")
    copies = [
        pltpu.make_async_copy(src, dst, sem.at[i])
        for i, (src, dst) in enumerate(((up_in, up_out), (down_in, down_out), (layer, layer_out)))
    ]
    copies[0].start()
    copies[1].start()

    @pl.loop(0, share // norm_tile)
    def _(m):
        here = pl.ds(pl.multiple_of(m * norm_tile, norm_tile), norm_tile)
        mine = pl.ds(pl.multiple_of(me * share + m * norm_tile, norm_tile), norm_tile)
        value = part[mine, :].astype(jnp.float32)
        for k in range(tp - 1):
            value = value + arrived[k, here, :].astype(jnp.float32)
        layer[here, :] = value.astype(jnp.bfloat16)

    copies[2].start()
    for copy in copies:
        copy.wait()


def on_device(prompt_rows, up_master, down_master, norm_gain):
    n = lax.axis_size("fs")
    tp = lax.axis_size("tp")
    bf16 = jnp.bfloat16
    up_rows, width = up_master.shape
    span = width // n
    fs_per_tp = n // tp
    up_width = fs_per_tp * span
    down_width = down_master.shape[1]
    if fs_per_tp > 1:
        up_master = up_master.reshape(up_rows, fs_per_tp, tp, span).swapaxes(1, 2)
        up_master = up_master.reshape(up_rows, width)
    groups = column_groups(tp, (up_width, down_width))
    count = len(groups)
    tokens, model = prompt_rows.shape
    units = n * span
    share = tokens // tp
    vmem = pl.BlockSpec(memory_space=pltpu.VMEM)
    hbm = pl.BlockSpec(memory_space=pl.ANY)
    dma = pltpu.SemaphoreType.DMA
    held = pl.pallas_call(
        functools.partial(gather_kernel, n, tp, groups),
        out_shape=(
            pltpu.VMEM((model, units), bf16),
            pltpu.VMEM((units, model), bf16),
            pltpu.VMEM((tokens, model), bf16),
            pltpu.VMEM((tp - 1, share, model), bf16),
        ),
        in_specs=[hbm, hbm, vmem, hbm],
        out_specs=(vmem, vmem, vmem, vmem),
        scratch_shapes=[
            pltpu.VMEM((tokens, model), bf16),
            pltpu.VMEM((tokens, units), bf16),
            pltpu.VMEM((tokens, groups[-1][3]), jnp.float32),
            pltpu.VMEM(up_master.shape, jnp.float32),
            pltpu.VMEM(down_master.shape, jnp.float32),
            pltpu.VMEM(up_master.shape, bf16),
            pltpu.VMEM(down_master.shape, bf16),
            pltpu.VMEM((up_rows, 128), jnp.float32),
            dma((tp + 3,)),
            dma((2,)),
            dma((2, tp - 1, 2)),
            dma((3,)),
            dma((count, n - 1)),
            dma((1,)),
            dma((count + pieces * n,)),
            dma((1,)),
            dma((1,)),
        ],
        compiler_params=pltpu.CompilerParams(
            collective_id=0, has_side_effects=True, vmem_limit_bytes=32 * 1024 * 1024
        ),
    )(up_master, down_master, norm_gain[None, :], prompt_rows)
    up_sampler, down_sampler, layer_out = pl.pallas_call(
        functools.partial(place_kernel, tp),
        out_shape=(
            jax.ShapeDtypeStruct((model, units), bf16),
            jax.ShapeDtypeStruct((units, model), bf16),
            jax.ShapeDtypeStruct((share, model), bf16),
        ),
        in_specs=[vmem] * 4,
        out_specs=(hbm, hbm, hbm),
        scratch_shapes=[pltpu.VMEM((share, model), bf16), dma((3,))],
        compiler_params=pltpu.CompilerParams(vmem_limit_bytes=8 * 1024 * 1024),
    )(*held)
    return (up_sampler[None], down_sampler[None], layer_out)


def solution(mesh):
    in_specs = (P(("grp", "fs"), None), P("fs", "tp"), P("fs", "tp"), P("fs"))
    out_specs = (
        P(("grp", "tp"), None, None),
        P(("grp", "tp"), None, None),
        P(("grp", "fs", "tp"), None),
    )
    return jax.shard_map(
        on_device, mesh=mesh, in_specs=in_specs, out_specs=out_specs, check_vma=False
    )
```

```python
import functools
import math

import jax
import jax.numpy as jnp
from jax import lax
from jax.experimental import pallas as pl
from jax.experimental.pallas import tpu as pltpu
from jax.sharding import PartitionSpec as P

eps = 1e-06
row_tile = 1024
norm_tile = 64
pieces = 2
MESH = pl.DeviceIdType.MESH


def column_groups(tp, widths):
    groups = []
    for w in range(2):
        for j in range(tp):
            width = 256 if widths[w] % 256 == 0 else widths[w]
            if w == 1 and j == tp - 1 and width == 256:
                width = 128
            for first in range(0, widths[w], width):
                groups.append((w, j, first, width))
    return groups


def own_plan(count, steps, ahead, behind):
    plan, sent = [], ahead
    early, late = count * 2 // 9, count * 2 // 3
    for step in range(steps):
        if step < early:
            lead = ahead
        elif step >= late:
            lead = behind
        else:
            lead = round(ahead + (behind - ahead) * (step - early + 1) / (late - early + 1))
        now = []
        while sent < count and (sent <= step + lead or step == steps - 1):
            now.append(sent)
            sent += 1
        plan.append(now)
    return plan


def gather_kernel(
    n, tp, groups, up_ref, down_ref, gain_ref, rows_ref, up_all, down_all, part, arrived,
    normed, hidden, total, up_stage, down_stage, up_cast, down_cast, gain_tall, load_sem,
    tp_send, tp_recv, z_send, z_recv, y_send, y_recv, sum_send, sum_recv,
):
    y = lax.axis_index("grp")
    z = lax.axis_index("fs")
    me = lax.axis_index("tp")
    chips = tp // 2
    depths = (up_ref.shape[0], down_ref.shape[0] // tp)
    widths = (up_ref.shape[1] // tp, down_ref.shape[1])
    alls = (up_all, down_all)
    tokens = rows_ref.shape[0]
    share = tokens // tp
    count = len(groups)
    first_down = sum(group[0] == 0 for group in groups)
    twins = n > 2
    lag = max(n - 2, 2)
    steps = count + lag
    ahead, lead = 2, 3
    plan = own_plan(count, steps, ahead, -1)
    middle = jnp.logical_and(z > 0, z < n - 1)

    def source(device, j):
        return lax.rem(device // 2 + j // 2, chips) * 2 + lax.rem(lax.rem(device, 2) + j % 2, 2)

    def target(j):
        return lax.rem(me // 2 + chips - j // 2, chips) * 2 + lax.rem(lax.rem(me, 2) + j % 2, 2)

    far_first = [k for k in range(2, tp)] + [1]

    def columns(g, b):
        w, _, first, width = groups[g]
        return pl.ds(pl.multiple_of(b * widths[w] + first, math.gcd(width, 256)), width)

    def rows(w, a, h):
        half = depths[w] // 2
        return pl.ds(pl.multiple_of(a * depths[w] + h * half, half), half)

    def block(g, a, h):
        w, j, _, _ = groups[g]
        return alls[w].at[rows(w, a, h), columns(g, source(me, j))]

    def wide(w, b):
        return pl.ds(pl.multiple_of(b * widths[w], widths[w]), widths[w])

    def remote(src, dst, send, recv, device):
        return pltpu.make_async_remote_copy(
            src_ref=src, dst_ref=dst, send_sem=send, recv_sem=recv,
            device_id=device, device_id_type=MESH,
        )

    def half_of(k):
        return y if k == 0 else 1 - y

    def tp_copy(w, j, k):
        half = depths[w] // 2
        t = target(j)
        if w == 0:
            src = up_cast.at[pl.ds(pl.multiple_of(half_of(k) * half, half), half), wide(0, t)]
        else:
            src = down_cast.at[pl.ds(pl.multiple_of(t * depths[1] + half_of(k) * half, half), half), :]
        dst = alls[w].at[rows(w, z, half_of(k)), wide(w, me)]
        return remote(src, dst, tp_send.at[w], tp_recv.at[w, j - 1, k], {"tp": t})

    def tp_arrival(w, j, k):
        ref = alls[w].at[rows(w, z, half_of(k)), wide(w, source(me, j))]
        return remote(ref, ref, tp_send.at[w], tp_recv.at[w, j - 1, k], {"tp": target(j)})

    def in_pieces(g):
        return groups[g][0] == 1 and g >= count - pieces and depths[1] % 128 == 0

    def half_sem(g, a):
        return y_recv.at[count + (g - count + pieces) * n + a if in_pieces(g) else g]

    def z_copy(g, a, way, device):
        ref = block(g, a, y)
        slot = lax.rem(a - device + n, n) - 1
        return remote(ref, ref, z_send.at[way], z_recv.at[g, slot], {"fs": device})

    def own_up(g):
        return z_copy(g, z, 0, z + 1)

    def own_down(g):
        return z_copy(g, z, 1, z - 1)

    def twin_copy(g, a, device):
        ref = block(g, a, 1 - y)
        return remote(ref, ref, z_send.at[2], half_sem(g, a), {"fs": device})

    def y_copy(g, a, h):
        ref = block(g, a, h)
        return remote(ref, ref, y_send.at[0], half_sem(g, a), {"grp": 1 - y})

    def sum_copy(g, k):
        t = target(k)
        cols = columns(g, source(me, groups[g][1]))
        src = part.at[pl.ds(pl.multiple_of(t * share, share), share), cols]
        return remote(src, arrived.at[k - 1, :, cols], sum_send.at[0], sum_recv.at[0], {"tp": t})

    def up_load(j):
        half = depths[0] // 2
        here = pl.ds(pl.multiple_of(y * half, half), half)
        cols = wide(0, target(j))
        return pltpu.make_async_copy(up_ref.at[here, cols], up_stage.at[here, cols], load_sem.at[j])

    def late_load():
        half = depths[0] // 2
        here = pl.ds(pl.multiple_of((1 - y) * half, half), half)
        return pltpu.make_async_copy(up_ref.at[here, :], up_stage.at[here, :], load_sem.at[tp])

    down_load = pltpu.make_async_copy(down_ref, down_stage, load_sem.at[tp + 1])
    rows_load = pltpu.make_async_copy(rows_ref, normed, load_sem.at[tp + 2])
    order = [0] + far_first
    for j in order:
        up_load(j).start()
    late_load().start()
    rows_load.start()
    down_load.start()
    barrier = pltpu.get_barrier_semaphore()
    for j in range(1, tp):
        pl.semaphore_signal(barrier, inc=1, device_id={"tp": target(j)}, device_id_type=MESH)
    pl.semaphore_signal(barrier, inc=1, device_id={"grp": 1 - y}, device_id_type=MESH)

    @pl.when(z > 0)
    def _():
        pl.semaphore_signal(barrier, inc=1, device_id={"fs": z - 1}, device_id_type=MESH)

    @pl.when(z < n - 1)
    def _():
        pl.semaphore_signal(barrier, inc=1, device_id={"fs": z + 1}, device_id_type=MESH)

    gain_tall[...] = jnp.broadcast_to(gain_ref[...], (128, depths[0])).T

    def cast_up(j, k):
        half = depths[0] // 2
        tile = math.gcd(half, norm_tile)
        cols = wide(0, target(j))

        @pl.loop(0, half // tile)
        def _(m):
            first = pl.multiple_of(half_of(k) * half + m * tile, tile)
            here = pl.ds(first, tile)
            value = (up_stage[here, cols] * gain_tall[here, :1]).astype(jnp.bfloat16)
            if j == 0:
                up_all[pl.ds(pl.multiple_of(z * depths[0] + first, tile), tile), cols] = value
            else:
                up_cast[here, cols] = value

    def cast_down():
        tile = math.gcd(depths[1], norm_tile)

        @pl.loop(0, down_ref.shape[0] // tile)
        def _(m):
            here = pl.ds(pl.multiple_of(m * tile, tile), tile)
            down_cast[here, :] = down_stage[here, :].astype(jnp.bfloat16)

        @pl.loop(0, depths[1] // tile)
        def _(m):
            here = pl.ds(pl.multiple_of(me * depths[1] + m * tile, tile), tile)
            there = pl.ds(pl.multiple_of(z * depths[1] + m * tile, tile), tile)
            down_all[there, wide(1, me)] = down_stage[here, :].astype(jnp.bfloat16)

    def norm_rows(first, many):
        @pl.loop(0, many // norm_tile)
        def _(m):
            here = pl.ds(pl.multiple_of(first + m * norm_tile, norm_tile), norm_tile)
            values = normed[here, :].astype(jnp.float32)
            scale = lax.rsqrt(jnp.mean(values * values, axis=-1, keepdims=True) + eps)
            normed[here, :] = (values * scale).astype(jnp.bfloat16)

    def late_own(g):
        @pl.when(z == 1)
        def _():
            own_down(g).start()

        @pl.when(z == n - 2)
        def _():
            own_up(g).start()

    def early_own(g):
        w, j, first, _ = groups[g]
        if j > 0 and first == 0:
            tp_arrival(w, j, 0).wait_recv()

        @pl.when(z > 1)
        def _():
            own_down(g).start()

        @pl.when(z < n - 2)
        def _():
            own_up(g).start()

    def twin_own(g):
        w, j, first, _ = groups[g]
        if j > 0 and first == 0:
            tp_arrival(w, j, 1).wait_recv()
        if twins:
            for edge, near in ((0, 1), (n - 1, n - 2)):

                @pl.when(z == edge)
                def _():
                    twin_copy(g, edge, near).start()

    def at_edge(body):
        for edge, way in ((0, 1), (n - 1, -1)):

            @pl.when(z == edge)
            def _():
                body(lambda s: edge + way * s)

    def edge_receive(g, a):
        z_copy(g, a, 0, z).wait_recv()
        y_copy(g, a, y).start()

    def receive(step):
        @pl.when(middle)
        def _():
            for s in range(1, n - 1):
                g = step - (s - 1)
                if not 0 <= g < count:
                    continue

                @pl.when(z >= s)
                def _():
                    a = z - s
                    z_copy(g, a, 0, z).wait_recv()
                    z_copy(g, a, 0, z + 1).start()
                    if s == 1 and twins:

                        @pl.when(a != 0)
                        def _():
                            y_copy(g, a, y).start()
                    else:
                        y_copy(g, a, y).start()

                @pl.when(z + s < n)
                def _():
                    a = z + s
                    z_copy(g, a, 0, z).wait_recv()
                    z_copy(g, a, 1, z - 1).start()
                    if s == 1 and twins:

                        @pl.when(a != n - 1)
                        def _():
                            y_copy(g, a, y).start()
                    else:
                        y_copy(g, a, y).start()

        def edge(at):
            for s in range(2, n):
                g = step - (s - 2)
                if 0 <= g < count:
                    edge_receive(g, at(s))
            for g in plan[step]:
                edge_receive(g, at(1))

        at_edge(edge)

    def other_half(g, a):
        y_copy(g, a, 1 - y).wait_recv()

    def other_halves(g):
        w = groups[g][0]
        half = depths[w] // 2
        ref = alls[w].at[pl.ds(0, (n - 1) * half), columns(g, source(me, groups[g][1]))]
        remote(ref, ref, y_send.at[0], y_recv.at[g], {"grp": 1 - y}).wait_recv()

    tile = math.gcd(tokens, row_tile)

    def finish(g):
        w, j, _, width = groups[g]
        cols = columns(g, source(me, j))

        def product(a, fresh):
            deep = pl.ds(pl.multiple_of(a * depths[1], depths[1]), depths[1])

            @pl.loop(0, tokens // tile)
            def _(m):
                here = pl.ds(pl.multiple_of(m * tile, tile), tile)
                acc = jnp.dot(hidden[here, deep], down_all[deep, cols], preferred_element_type=jnp.float32)
                total[here, :] = acc if fresh else total[here, :] + acc

        if in_pieces(g):
            product(z, True)
            for s in [*range(2, n), 1]:
                for a in range(n):
                    if a - s < 0 and a + s > n - 1:
                        continue
                    near = z - a == s if a + s < n else a - z == s
                    if a + s < n and a - s >= 0:
                        near = jnp.logical_or(z - a == s, a - z == s)

                    @pl.when(near)
                    def _():
                        other_half(g, a)
                        product(a, False)

            @pl.loop(0, tokens // tile)
            def _(m):
                here = pl.ds(pl.multiple_of(m * tile, tile), tile)
                part[here, cols] = total[here, :].astype(jnp.bfloat16)
        else:
            other_halves(g)

            @pl.loop(0, tokens // tile)
            def _(m):
                here = pl.ds(pl.multiple_of(m * tile, tile), tile)
                if w == 0:
                    acc = jnp.dot(normed[here, :], up_all[:, cols], preferred_element_type=jnp.float32)
                    acc = jnp.maximum(acc, 0.0)
                    hidden[here, cols] = (acc * acc).astype(jnp.bfloat16)
                else:
                    acc = jnp.dot(hidden[here, :], down_all[:, cols], preferred_element_type=jnp.float32)
                    part[here, cols] = acc.astype(jnp.bfloat16)

        if w == 1:
            for k in far_first:
                sum_copy(g, k).start()

    up_load(0).wait()
    cast_up(0, 0)
    pl.semaphore_wait(barrier, tp + (z + n - 1) // n + (2 * n - 2 - z) // n)
    for g in range(ahead):
        early_own(g)
        late_own(g)
    for j in far_first:
        up_load(j).wait()
        cast_up(j, 0)
        tp_copy(0, j, 0).start()
    late_load().wait()
    for j in far_first + [0]:
        cast_up(j, 1)
        if j > 0:
            tp_copy(0, j, 1).start()
    rows_load.wait()
    quarter = tokens // 4

    def down_work():
        down_load.wait()
        cast_down()
        for k in range(2):
            for j in far_first:
                tp_copy(1, j, k).start()

    work = [functools.partial(norm_rows, i * quarter, quarter) for i in range(4)] + [down_work]
    for g in range(ahead):
        at_edge(lambda at: edge_receive(g, at(1)))
        work.pop(0)()
    sent = ahead
    for step in range(steps):
        receive(step)
        while sent < count and sent <= step + lead:
            early_own(sent)
            sent += 1
        for g in plan[step]:
            late_own(g)
        if step < count:
            twin_own(step)
        if work:
            work.pop(0)()
        if step >= lag:
            while work:
                work.pop(0)()
            finish(step - lag)

    def await_sends(ref, sem):
        remote(ref, ref, sem, sum_recv.at[0], {"grp": 1 - y}).wait_send()

    await_sends(up_cast.at[:, pl.ds(0, (tp - 1) * widths[0])], tp_send.at[0])
    await_sends(down_cast.at[pl.ds(0, (tp - 1) * depths[1]), :], tp_send.at[1])
    for edge in range(n):
        passed = n - 1 - (twins and edge == 1) - (twins and edge == n - 2)
        waits = [
            (z_send.at[0], edge + 1 if edge < n - 1 else 0),
            (z_send.at[1], n - edge if edge > 0 else 0),
            (z_send.at[2], int(twins and edge in (0, n - 1))),
            (y_send.at[0], passed),
        ]

        @pl.when(z == edge)
        def _():
            for sem, blocks in waits:
                if blocks:
                    await_sends(up_all.at[pl.ds(0, blocks * depths[0]), :], sem)

    remote(arrived, arrived, sum_send.at[0], sum_recv.at[0], {"grp": 1 - y}).wait()


def place_kernel(tp, up_in, down_in, part, arrived, up_out, down_out, layer_out, layer, sem):
    share = layer.shape[0]
    me = lax.axis_index("tp")
    copies = [
        pltpu.make_async_copy(src, dst, sem.at[i])
        for i, (src, dst) in enumerate(((up_in, up_out), (down_in, down_out), (layer, layer_out)))
    ]
    copies[0].start()
    copies[1].start()

    @pl.loop(0, share // norm_tile)
    def _(m):
        here = pl.ds(pl.multiple_of(m * norm_tile, norm_tile), norm_tile)
        mine = pl.ds(pl.multiple_of(me * share + m * norm_tile, norm_tile), norm_tile)
        value = part[mine, :].astype(jnp.float32)
        for k in range(tp - 1):
            value = value + arrived[k, here, :].astype(jnp.float32)
        layer[here, :] = value.astype(jnp.bfloat16)

    copies[2].start()
    for copy in copies:
        copy.wait()


def on_device(prompt_rows, up_master, down_master, norm_gain):
    n = lax.axis_size("fs")
    tp = lax.axis_size("tp")
    bf16 = jnp.bfloat16
    up_rows, width = up_master.shape
    span = width // n
    fs_per_tp = n // tp
    up_width = fs_per_tp * span
    down_width = down_master.shape[1]
    if fs_per_tp > 1:
        up_master = up_master.reshape(up_rows, fs_per_tp, tp, span).swapaxes(1, 2)
        up_master = up_master.reshape(up_rows, width)
    groups = column_groups(tp, (up_width, down_width))
    count = len(groups)
    tokens, model = prompt_rows.shape
    units = n * span
    share = tokens // tp
    vmem = pl.BlockSpec(memory_space=pltpu.VMEM)
    hbm = pl.BlockSpec(memory_space=pl.ANY)
    dma = pltpu.SemaphoreType.DMA
    held = pl.pallas_call(
        functools.partial(gather_kernel, n, tp, groups),
        out_shape=(
            pltpu.VMEM((model, units), bf16),
            pltpu.VMEM((units, model), bf16),
            pltpu.VMEM((tokens, model), bf16),
            pltpu.VMEM((tp - 1, share, model), bf16),
        ),
        in_specs=[hbm, hbm, vmem, hbm],
        out_specs=(vmem, vmem, vmem, vmem),
        scratch_shapes=[
            pltpu.VMEM((tokens, model), bf16),
            pltpu.VMEM((tokens, units), bf16),
            pltpu.VMEM((tokens, groups[-1][3]), jnp.float32),
            pltpu.VMEM(up_master.shape, jnp.float32),
            pltpu.VMEM(down_master.shape, jnp.float32),
            pltpu.VMEM(up_master.shape, bf16),
            pltpu.VMEM(down_master.shape, bf16),
            pltpu.VMEM((up_rows, 128), jnp.float32),
            dma((tp + 3,)),
            dma((2,)),
            dma((2, tp - 1, 2)),
            dma((3,)),
            dma((count, n - 1)),
            dma((1,)),
            dma((count + pieces * n,)),
            dma((1,)),
            dma((1,)),
        ],
        compiler_params=pltpu.CompilerParams(
            collective_id=0, has_side_effects=True, vmem_limit_bytes=32 * 1024 * 1024
        ),
    )(up_master, down_master, norm_gain[None, :], prompt_rows)
    up_sampler, down_sampler, layer_out = pl.pallas_call(
        functools.partial(place_kernel, tp),
        out_shape=(
            jax.ShapeDtypeStruct((model, units), bf16),
            jax.ShapeDtypeStruct((units, model), bf16),
            jax.ShapeDtypeStruct((share, model), bf16),
        ),
        in_specs=[vmem] * 4,
        out_specs=(hbm, hbm, hbm),
        scratch_shapes=[pltpu.VMEM((share, model), bf16), dma((3,))],
        compiler_params=pltpu.CompilerParams(vmem_limit_bytes=8 * 1024 * 1024),
    )(*held)
    return (up_sampler[None], down_sampler[None], layer_out)


def solution(mesh):
    in_specs = (P(("grp", "fs"), None), P("fs", "tp"), P("fs", "tp"), P("fs"))
    out_specs = (
        P(("grp", "tp"), None, None),
        P(("grp", "tp"), None, None),
        P(("grp", "fs", "tp"), None),
    )
    return jax.shard_map(
        on_device, mesh=mesh, in_specs=in_specs, out_specs=out_specs, check_vma=False
    )
```

```python
import functools
import math

import jax
import jax.numpy as jnp
from jax import lax
from jax.experimental import pallas as pl
from jax.experimental.pallas import tpu as pltpu
from jax.sharding import PartitionSpec as P

eps = 1e-06
row_tile = 1024
step_rows = 512
norm_tile = 64
pieces = 4
final_twins = 2
MESH = pl.DeviceIdType.MESH


def column_groups(tp, widths):
    groups = []
    for w in range(2):
        for j in range(tp):
            width = 256 if widths[w] % 256 == 0 else widths[w]
            if w == 1 and j == tp - 1 and width == 256:
                width = 128
            for first in range(0, widths[w], width):
                groups.append((w, j, first, width))
    return groups


def own_plan(count, steps, ahead, behind):
    plan, sent = [], ahead
    early, late = count * 2 // 9, count * 2 // 3
    for step in range(steps):
        if step < early:
            lead = ahead
        elif step >= late:
            lead = behind
        else:
            lead = round(ahead + (behind - ahead) * (step - early + 1) / (late - early + 1))
        now = []
        while sent < count and (sent <= step + lead or step == steps - 1):
            now.append(sent)
            sent += 1
        plan.append(now)
    return plan


def gather_kernel(
    n, tp, groups, up_ref, down_ref, gain_ref, rows_ref, up_all, down_all, part, arrived,
    normed, hidden, total, up_stage, down_stage, up_cast, down_cast, gain_tall, load_sem,
    tp_send, tp_recv, z_send, z_recv, y_send, y_recv, sum_send, sum_recv,
):
    y = lax.axis_index("grp")
    z = lax.axis_index("fs")
    me = lax.axis_index("tp")
    chips = tp // 2
    depths = (up_ref.shape[0], down_ref.shape[0] // tp)
    widths = (up_ref.shape[1] // tp, down_ref.shape[1])
    alls = (up_all, down_all)
    tokens = rows_ref.shape[0]
    model = down_all.shape[1]
    share = tokens // tp
    count = len(groups)
    first_down = sum(group[0] == 0 for group in groups)
    twins = n > 2
    doubled = range(count - final_twins, count) if twins and depths[1] % 128 == 0 else range(0)
    spare = sum(groups[g][3] for g in doubled)
    lag = max(n - 2, 2)
    steps = count + lag
    ahead, lead = 2, 3
    plan = own_plan(count, steps, ahead, -1)
    middle = jnp.logical_and(z > 0, z < n - 1)

    def source(device, j):
        return lax.rem(device // 2 + j // 2, chips) * 2 + lax.rem(lax.rem(device, 2) + j % 2, 2)

    def target(j):
        return lax.rem(me // 2 + chips - j // 2, chips) * 2 + lax.rem(lax.rem(me, 2) + j % 2, 2)

    far_first = [k for k in range(2, tp)] + [1]

    def columns(g, b):
        w, _, first, width = groups[g]
        return pl.ds(pl.multiple_of(b * widths[w] + first, math.gcd(width, 256)), width)

    def rows(w, a, h):
        half = depths[w] // 2
        return pl.ds(pl.multiple_of(a * depths[w] + h * half, half), half)

    def block(g, a, h):
        w, j, _, _ = groups[g]
        return alls[w].at[rows(w, a, h), columns(g, source(me, j))]

    def wide(w, b):
        return pl.ds(pl.multiple_of(b * widths[w], widths[w]), widths[w])

    def remote(src, dst, send, recv, device):
        return pltpu.make_async_remote_copy(
            src_ref=src, dst_ref=dst, send_sem=send, recv_sem=recv,
            device_id=device, device_id_type=MESH,
        )

    def half_of(k):
        return y if k == 0 else 1 - y

    def tp_copy(w, j, k):
        half = depths[w] // 2
        t = target(j)
        if w == 0:
            src = up_cast.at[pl.ds(pl.multiple_of(half_of(k) * half, half), half), wide(0, t)]
        else:
            src = down_cast.at[pl.ds(pl.multiple_of(t * depths[1] + half_of(k) * half, half), half), :]
        dst = alls[w].at[rows(w, z, half_of(k)), wide(w, me)]
        return remote(src, dst, tp_send.at[w], tp_recv.at[w, j - 1, k], {"tp": t})

    def tp_arrival(w, j, k):
        ref = alls[w].at[rows(w, z, half_of(k)), wide(w, source(me, j))]
        return remote(ref, ref, tp_send.at[w], tp_recv.at[w, j - 1, k], {"tp": target(j)})

    def in_pieces(g):
        return groups[g][0] == 1 and g >= count - pieces and depths[1] % 128 == 0

    def half_sem(g, a):
        return y_recv.at[count + (g - count + pieces) * n + a if in_pieces(g) else g]

    def half_sent(g):
        return y_send.at[2 if g in doubled else groups[g][0]]

    def z_copy(g, a, way, device):
        ref = block(g, a, y)
        slot = lax.rem(a - device + n, n) - 1
        return remote(ref, ref, z_send.at[way], z_recv.at[g, slot], {"fs": device})

    def own_up(g):
        return z_copy(g, z, 0, z + 1)

    def own_down(g):
        return z_copy(g, z, 1, z - 1)

    def twin_copy(g, a, way, device):
        ref = block(g, a, 1 - y)
        return remote(ref, ref, z_send.at[way], half_sem(g, a), {"fs": device})

    def y_copy(g, a, h):
        ref = block(g, a, h)
        return remote(ref, ref, half_sent(g), half_sem(g, a), {"grp": 1 - y})

    def sum_copy(g, k):
        t = target(k)
        cols = columns(g, source(me, groups[g][1]))
        src = part.at[pl.ds(pl.multiple_of(t * share, share), share), cols]
        return remote(src, arrived.at[k - 1, :, cols], sum_send.at[0], sum_recv.at[0], {"tp": t})

    def up_load(j):
        half = depths[0] // 2
        here = pl.ds(pl.multiple_of(y * half, half), half)
        cols = wide(0, target(j))
        return pltpu.make_async_copy(up_ref.at[here, cols], up_stage.at[here, cols], load_sem.at[j])

    def late_load():
        half = depths[0] // 2
        here = pl.ds(pl.multiple_of((1 - y) * half, half), half)
        return pltpu.make_async_copy(up_ref.at[here, :], up_stage.at[here, :], load_sem.at[tp])

    down_load = pltpu.make_async_copy(down_ref, down_stage, load_sem.at[tp + 1])
    rows_load = pltpu.make_async_copy(rows_ref, normed, load_sem.at[tp + 2])
    order = [0] + far_first
    for j in order:
        up_load(j).start()
    late_load().start()
    rows_load.start()
    down_load.start()
    barrier = pltpu.get_barrier_semaphore()
    for j in range(1, tp):
        pl.semaphore_signal(barrier, inc=1, device_id={"tp": target(j)}, device_id_type=MESH)
    pl.semaphore_signal(barrier, inc=1, device_id={"grp": 1 - y}, device_id_type=MESH)

    @pl.when(z > 0)
    def _():
        pl.semaphore_signal(barrier, inc=1, device_id={"fs": z - 1}, device_id_type=MESH)

    @pl.when(z < n - 1)
    def _():
        pl.semaphore_signal(barrier, inc=1, device_id={"fs": z + 1}, device_id_type=MESH)

    gain_tall[...] = jnp.broadcast_to(gain_ref[...], (128, depths[0])).T

    def cast_up(j, k):
        half = depths[0] // 2
        tile = math.gcd(half, norm_tile)
        cols = wide(0, target(j))

        @pl.loop(0, half // tile)
        def _(m):
            first = pl.multiple_of(half_of(k) * half + m * tile, tile)
            here = pl.ds(first, tile)
            value = (up_stage[here, cols] * gain_tall[here, :1]).astype(jnp.bfloat16)
            if j == 0:
                up_all[pl.ds(pl.multiple_of(z * depths[0] + first, tile), tile), cols] = value
            else:
                up_cast[here, cols] = value

    def cast_down():
        tile = math.gcd(depths[1], norm_tile)

        @pl.loop(0, down_ref.shape[0] // tile)
        def _(m):
            here = pl.ds(pl.multiple_of(m * tile, tile), tile)
            down_cast[here, :] = down_stage[here, :].astype(jnp.bfloat16)

        @pl.loop(0, depths[1] // tile)
        def _(m):
            here = pl.ds(pl.multiple_of(me * depths[1] + m * tile, tile), tile)
            there = pl.ds(pl.multiple_of(z * depths[1] + m * tile, tile), tile)
            down_all[there, wide(1, me)] = down_stage[here, :].astype(jnp.bfloat16)

    def norm_rows(first, many):
        @pl.loop(0, many // norm_tile)
        def _(m):
            here = pl.ds(pl.multiple_of(first + m * norm_tile, norm_tile), norm_tile)
            values = normed[here, :].astype(jnp.float32)
            scale = lax.rsqrt(jnp.mean(values * values, axis=-1, keepdims=True) + eps)
            normed[here, :] = (values * scale).astype(jnp.bfloat16)

    def late_own(g):
        @pl.when(z == 1)
        def _():
            own_down(g).start()
            if g in doubled:
                twin_copy(g, 1, 3, 0).start()

        @pl.when(z == n - 2)
        def _():
            own_up(g).start()
            if g in doubled:
                twin_copy(g, n - 2, 3 if n > 3 else 4, n - 1).start()

    def early_own(g):
        w, j, first, _ = groups[g]
        if j > 0 and first == 0:
            tp_arrival(w, j, 0).wait_recv()

        @pl.when(z > 1)
        def _():
            own_down(g).start()

        @pl.when(z < n - 2)
        def _():
            own_up(g).start()

    def twin_own(g):
        w, j, first, _ = groups[g]
        if j > 0 and first == 0:
            tp_arrival(w, j, 1).wait_recv()
        if twins:
            for edge, near in ((0, 1), (n - 1, n - 2)):

                @pl.when(z == edge)
                def _():
                    twin_copy(g, edge, 2, near).start()

    def at_edge(body):
        for edge, way in ((0, 1), (n - 1, -1)):

            @pl.when(z == edge)
            def _():
                body(lambda s: edge + way * s)

    def edge_receive(g, a, whole=False):
        z_copy(g, a, 0, z).wait_recv()
        if not whole:
            y_copy(g, a, y).start()

    def receive_near(step):
        def edge(at):
            for g in plan[step]:
                edge_receive(g, at(1), g in doubled)

        at_edge(edge)

    def receive(step):
        @pl.when(middle)
        def _():
            for s in range(1, n - 1):
                g = step - (s - 1)
                if not 0 <= g < count:
                    continue

                @pl.when(z >= s)
                def _():
                    a = z - s
                    z_copy(g, a, 0, z).wait_recv()
                    z_copy(g, a, 0, z + 1).start()
                    if s == 1 and twins:

                        @pl.when(a != 0)
                        def _():
                            y_copy(g, a, y).start()
                    else:
                        y_copy(g, a, y).start()

                @pl.when(z + s < n)
                def _():
                    a = z + s
                    z_copy(g, a, 0, z).wait_recv()
                    z_copy(g, a, 1, z - 1).start()
                    if s == 1 and twins:

                        @pl.when(a != n - 1)
                        def _():
                            y_copy(g, a, y).start()
                    else:
                        y_copy(g, a, y).start()

        def edge(at):
            for s in range(2, n):
                g = step - (s - 2)
                if 0 <= g < count:
                    edge_receive(g, at(s))

        at_edge(edge)

    def other_half(g, a):
        y_copy(g, a, 1 - y).wait_recv()

    def other_halves(g):
        w = groups[g][0]
        half = depths[w] // 2
        ref = alls[w].at[pl.ds(0, (n - 1) * half), columns(g, source(me, groups[g][1]))]
        remote(ref, ref, half_sent(g), y_recv.at[g], {"grp": 1 - y}).wait_recv()

    tile = math.gcd(tokens, row_tile)
    step_tile = math.gcd(tokens, step_rows)

    def finish(g):
        w, j, _, width = groups[g]
        cols = columns(g, source(me, j))

        def product(a, fresh):
            deep = pl.ds(pl.multiple_of(a * depths[1], depths[1]), depths[1])

            @pl.loop(0, tokens // tile)
            def _(m):
                here = pl.ds(pl.multiple_of(m * tile, tile), tile)
                acc = jnp.dot(hidden[here, deep], down_all[deep, cols], preferred_element_type=jnp.float32)
                total[here, :] = acc if fresh else total[here, :] + acc

        if in_pieces(g):
            product(z, True)

            @pl.loop(1, n)
            def _(i):
                turn = jnp.where(i == n - 1, 1, i + 1)
                a = lax.rem(jnp.where(2 * z < n, z + turn, z - turn + n), n)
                other_half(g, a)
                product(a, False)

            @pl.loop(0, tokens // tile)
            def _(m):
                here = pl.ds(pl.multiple_of(m * tile, tile), tile)
                part[here, cols] = total[here, :].astype(jnp.bfloat16)
        else:
            other_halves(g)

            @pl.loop(0, tokens // step_tile)
            def _(m):
                here = pl.ds(pl.multiple_of(m * step_tile, step_tile), step_tile)
                if w == 0:
                    acc = jnp.dot(normed[here, :], up_all[:, cols], preferred_element_type=jnp.float32)
                    acc = jnp.maximum(acc, 0.0)
                    hidden[here, cols] = (acc * acc).astype(jnp.bfloat16)
                else:
                    acc = jnp.dot(hidden[here, :], down_all[:, cols], preferred_element_type=jnp.float32)
                    part[here, cols] = acc.astype(jnp.bfloat16)

        if w == 1:
            for k in far_first:
                sum_copy(g, k).start()

    up_load(0).wait()
    cast_up(0, 0)
    pl.semaphore_wait(barrier, tp + (z + n - 1) // n + (2 * n - 2 - z) // n)
    for g in range(ahead):
        early_own(g)
        late_own(g)
    for j in far_first:
        up_load(j).wait()
        cast_up(j, 0)
        tp_copy(0, j, 0).start()
    late_load().wait()
    for j in far_first + [0]:
        cast_up(j, 1)
        if j > 0:
            tp_copy(0, j, 1).start()
    rows_load.wait()
    quarter = tokens // 4

    def down_work():
        down_load.wait()
        cast_down()
        for k in range(2):
            for j in far_first:
                tp_copy(1, j, k).start()

    work = [functools.partial(norm_rows, i * quarter, quarter) for i in range(4)] + [down_work]
    for g in range(ahead):
        at_edge(lambda at: edge_receive(g, at(1)))
        work.pop(0)()
    sent = ahead
    for step in range(steps):
        receive(step)
        if step < first_down + lag:
            receive_near(step)
        while sent < count and sent <= step + lead:
            early_own(sent)
            sent += 1
        for g in plan[step]:
            late_own(g)
        if step < count:
            twin_own(step)
        if work:
            work.pop(0)()
        if step >= lag:
            while work:
                work.pop(0)()
            finish(step - lag)
        if step >= first_down + lag:
            receive_near(step)

    def await_sends(ref, sem):
        remote(ref, ref, sem, sum_recv.at[0], {"grp": 1 - y}).wait_send()

    await_sends(up_cast.at[:, pl.ds(0, (tp - 1) * widths[0])], tp_send.at[0])
    await_sends(down_cast.at[pl.ds(0, (tp - 1) * depths[1]), :], tp_send.at[1])
    halves = [depth // 2 for depth in depths]
    for at in range(n):
        passed = n - 1 - (twins and at == 1) - (twins and at == n - 2)
        up_blocks = at + 1 if at < n - 1 else 0
        down_blocks = n - at if at > 0 else 0
        unequal = passed - (at in (0, n - 1))

        @pl.when(z == at)
        def _():
            if up_blocks:
                await_sends(up_all.at[pl.ds(0, up_blocks * depths[0]), :], z_send.at[0])
            if down_blocks:
                await_sends(up_all.at[pl.ds(0, down_blocks * depths[0]), :], z_send.at[1])
            if twins and at in (0, n - 1):
                await_sends(up_all.at[pl.ds(0, depths[0]), :], z_send.at[2])
            if spare and at == 1:
                await_sends(down_all.at[pl.ds(0, halves[1]), pl.ds(0, spare)], z_send.at[3])
            if spare and at == n - 2:
                way = 3 if n > 3 else 4
                await_sends(down_all.at[pl.ds(0, halves[1]), pl.ds(0, spare)], z_send.at[way])
            if passed:
                await_sends(up_all.at[pl.ds(0, passed * halves[0]), :], y_send.at[0])
                rest = pl.ds(0, model - spare)
                await_sends(down_all.at[pl.ds(0, passed * halves[1]), rest], y_send.at[1])
            if spare and unequal:
                await_sends(down_all.at[pl.ds(0, unequal * halves[1]), pl.ds(0, spare)], y_send.at[2])

    remote(arrived, arrived, sum_send.at[0], sum_recv.at[0], {"grp": 1 - y}).wait()


def place_kernel(tp, up_in, down_in, part, arrived, up_out, down_out, layer_out, layer, sem):
    share = layer.shape[0]
    me = lax.axis_index("tp")
    copies = [
        pltpu.make_async_copy(src, dst, sem.at[i])
        for i, (src, dst) in enumerate(((up_in, up_out), (down_in, down_out), (layer, layer_out)))
    ]
    copies[0].start()
    copies[1].start()

    @pl.loop(0, share // norm_tile)
    def _(m):
        here = pl.ds(pl.multiple_of(m * norm_tile, norm_tile), norm_tile)
        mine = pl.ds(pl.multiple_of(me * share + m * norm_tile, norm_tile), norm_tile)
        value = part[mine, :].astype(jnp.float32)
        for k in range(tp - 1):
            value = value + arrived[k, here, :].astype(jnp.float32)
        layer[here, :] = value.astype(jnp.bfloat16)

    copies[2].start()
    for copy in copies:
        copy.wait()


def on_device(prompt_rows, up_master, down_master, norm_gain):
    n = lax.axis_size("fs")
    tp = lax.axis_size("tp")
    bf16 = jnp.bfloat16
    up_rows, width = up_master.shape
    span = width // n
    fs_per_tp = n // tp
    up_width = fs_per_tp * span
    down_width = down_master.shape[1]
    if fs_per_tp > 1:
        up_master = up_master.reshape(up_rows, fs_per_tp, tp, span).swapaxes(1, 2)
        up_master = up_master.reshape(up_rows, width)
    groups = column_groups(tp, (up_width, down_width))
    count = len(groups)
    tokens, model = prompt_rows.shape
    units = n * span
    share = tokens // tp
    vmem = pl.BlockSpec(memory_space=pltpu.VMEM)
    hbm = pl.BlockSpec(memory_space=pl.ANY)
    dma = pltpu.SemaphoreType.DMA
    held = pl.pallas_call(
        functools.partial(gather_kernel, n, tp, groups),
        out_shape=(
            pltpu.VMEM((model, units), bf16),
            pltpu.VMEM((units, model), bf16),
            pltpu.VMEM((tokens, model), bf16),
            pltpu.VMEM((tp - 1, share, model), bf16),
        ),
        in_specs=[hbm, hbm, vmem, hbm],
        out_specs=(vmem, vmem, vmem, vmem),
        scratch_shapes=[
            pltpu.VMEM((tokens, model), bf16),
            pltpu.VMEM((tokens, units), bf16),
            pltpu.VMEM((tokens, groups[-1][3]), jnp.float32),
            pltpu.VMEM(up_master.shape, jnp.float32),
            pltpu.VMEM(down_master.shape, jnp.float32),
            pltpu.VMEM(up_master.shape, bf16),
            pltpu.VMEM(down_master.shape, bf16),
            pltpu.VMEM((up_rows, 128), jnp.float32),
            dma((tp + 3,)),
            dma((2,)),
            dma((2, tp - 1, 2)),
            dma((5,)),
            dma((count, n - 1)),
            dma((3,)),
            dma((count + pieces * n,)),
            dma((1,)),
            dma((1,)),
        ],
        compiler_params=pltpu.CompilerParams(
            collective_id=0, has_side_effects=True, vmem_limit_bytes=32 * 1024 * 1024
        ),
    )(up_master, down_master, norm_gain[None, :], prompt_rows)
    up_sampler, down_sampler, layer_out = pl.pallas_call(
        functools.partial(place_kernel, tp),
        out_shape=(
            jax.ShapeDtypeStruct((model, units), bf16),
            jax.ShapeDtypeStruct((units, model), bf16),
            jax.ShapeDtypeStruct((share, model), bf16),
        ),
        in_specs=[vmem] * 4,
        out_specs=(hbm, hbm, hbm),
        scratch_shapes=[pltpu.VMEM((share, model), bf16), dma((3,))],
        compiler_params=pltpu.CompilerParams(vmem_limit_bytes=8 * 1024 * 1024),
    )(*held)
    return (up_sampler[None], down_sampler[None], layer_out)


def solution(mesh):
    in_specs = (P(("grp", "fs"), None), P("fs", "tp"), P("fs", "tp"), P("fs"))
    out_specs = (
        P(("grp", "tp"), None, None),
        P(("grp", "tp"), None, None),
        P(("grp", "fs", "tp"), None),
    )
    return jax.shard_map(
        on_device, mesh=mesh, in_specs=in_specs, out_specs=out_specs, check_vma=False
    )
```

```python
import functools
import math

import jax
import jax.numpy as jnp
from jax import lax
from jax.experimental import pallas as pl
from jax.experimental.pallas import tpu as pltpu
from jax.sharding import PartitionSpec as P

eps = 1e-06
row_tile = 1024
step_rows = 256
norm_tile = 64
pieces = 4
final_twins = 2
MESH = pl.DeviceIdType.MESH


def column_groups(tp, widths):
    groups = []
    for w in range(2):
        for j in range(tp):
            width = 256 if widths[w] % 256 == 0 else widths[w]
            if w == 1 and j == tp - 1 and width == 256:
                width = 128
            for first in range(0, widths[w], width):
                groups.append((w, j, first, width))
    return groups


def own_plan(count, steps, ahead, behind):
    plan, sent = [], ahead
    early, late = count * 2 // 9, count * 2 // 3
    for step in range(steps):
        if step < early:
            lead = ahead
        elif step >= late:
            lead = behind
        else:
            lead = round(ahead + (behind - ahead) * (step - early + 1) / (late - early + 1))
        now = []
        while sent < count and (sent <= step + lead or step == steps - 1):
            now.append(sent)
            sent += 1
        plan.append(now)
    return plan


def gather_kernel(
    n, tp, groups, up_ref, down_ref, gain_ref, rows_ref, up_all, down_all, part, arrived,
    normed, hidden, total, up_stage, down_stage, up_cast, down_cast, gain_tall, load_sem,
    tp_send, tp_recv, z_send, z_recv, y_send, y_recv, sum_send, sum_recv,
):
    y = lax.axis_index("grp")
    z = lax.axis_index("fs")
    me = lax.axis_index("tp")
    chips = tp // 2
    depths = (up_ref.shape[0], down_ref.shape[0] // tp)
    widths = (up_ref.shape[1] // tp, down_ref.shape[1])
    alls = (up_all, down_all)
    tokens = rows_ref.shape[0]
    model = down_all.shape[1]
    share = tokens // tp
    count = len(groups)
    first_down = sum(group[0] == 0 for group in groups)
    twins = n > 2
    doubled = range(count - final_twins, count) if twins and depths[1] % 128 == 0 else range(0)
    spare = sum(groups[g][3] for g in doubled)
    lag = max(n - 2, 2)
    steps = count + lag
    ahead, lead = 2, 3
    plan = own_plan(count, steps, ahead, -1)
    middle = jnp.logical_and(z > 0, z < n - 1)

    def source(device, j):
        return lax.rem(device // 2 + j // 2, chips) * 2 + lax.rem(lax.rem(device, 2) + j % 2, 2)

    def target(j):
        return lax.rem(me // 2 + chips - j // 2, chips) * 2 + lax.rem(lax.rem(me, 2) + j % 2, 2)

    far_first = [k for k in range(2, tp)] + [1]

    def columns(g, b):
        w, _, first, width = groups[g]
        return pl.ds(pl.multiple_of(b * widths[w] + first, math.gcd(width, 256)), width)

    def rows(w, a, h):
        half = depths[w] // 2
        return pl.ds(pl.multiple_of(a * depths[w] + h * half, half), half)

    def block(g, a, h):
        w, j, _, _ = groups[g]
        return alls[w].at[rows(w, a, h), columns(g, source(me, j))]

    def wide(w, b):
        return pl.ds(pl.multiple_of(b * widths[w], widths[w]), widths[w])

    def remote(src, dst, send, recv, device):
        return pltpu.make_async_remote_copy(
            src_ref=src, dst_ref=dst, send_sem=send, recv_sem=recv,
            device_id=device, device_id_type=MESH,
        )

    def half_of(k):
        return y if k == 0 else 1 - y

    def tp_copy(w, j, k):
        half = depths[w] // 2
        t = target(j)
        if w == 0:
            src = up_cast.at[pl.ds(pl.multiple_of(half_of(k) * half, half), half), wide(0, t)]
        else:
            src = down_cast.at[pl.ds(pl.multiple_of(t * depths[1] + half_of(k) * half, half), half), :]
        dst = alls[w].at[rows(w, z, half_of(k)), wide(w, me)]
        return remote(src, dst, tp_send.at[w], tp_recv.at[w, j - 1, k], {"tp": t})

    def tp_arrival(w, j, k):
        ref = alls[w].at[rows(w, z, half_of(k)), wide(w, source(me, j))]
        return remote(ref, ref, tp_send.at[w], tp_recv.at[w, j - 1, k], {"tp": target(j)})

    def in_pieces(g):
        return groups[g][0] == 1 and g >= count - pieces and depths[1] % 128 == 0

    def half_sem(g, a):
        return y_recv.at[count + (g - count + pieces) * n + a if in_pieces(g) else g]

    def half_sent(g):
        return y_send.at[2 if g in doubled else groups[g][0]]

    def z_copy(g, a, way, device):
        ref = block(g, a, y)
        slot = lax.rem(a - device + n, n) - 1
        return remote(ref, ref, z_send.at[way], z_recv.at[g, slot], {"fs": device})

    def own_up(g):
        return z_copy(g, z, 0, z + 1)

    def own_down(g):
        return z_copy(g, z, 1, z - 1)

    def twin_copy(g, a, way, device):
        ref = block(g, a, 1 - y)
        return remote(ref, ref, z_send.at[way], half_sem(g, a), {"fs": device})

    def y_copy(g, a, h):
        ref = block(g, a, h)
        return remote(ref, ref, half_sent(g), half_sem(g, a), {"grp": 1 - y})

    def sum_copy(g, k):
        t = target(k)
        cols = columns(g, source(me, groups[g][1]))
        src = part.at[pl.ds(pl.multiple_of(t * share, share), share), cols]
        return remote(src, arrived.at[k - 1, :, cols], sum_send.at[0], sum_recv.at[0], {"tp": t})

    def up_load(j):
        half = depths[0] // 2
        here = pl.ds(pl.multiple_of(y * half, half), half)
        cols = wide(0, target(j))
        return pltpu.make_async_copy(up_ref.at[here, cols], up_stage.at[here, cols], load_sem.at[j])

    def late_load():
        half = depths[0] // 2
        here = pl.ds(pl.multiple_of((1 - y) * half, half), half)
        return pltpu.make_async_copy(up_ref.at[here, :], up_stage.at[here, :], load_sem.at[tp])

    down_load = pltpu.make_async_copy(down_ref, down_stage, load_sem.at[tp + 1])
    rows_load = pltpu.make_async_copy(rows_ref, normed, load_sem.at[tp + 2])
    order = [0] + far_first
    for j in order:
        up_load(j).start()
    late_load().start()
    rows_load.start()
    down_load.start()
    barrier = pltpu.get_barrier_semaphore()
    for j in range(1, tp):
        pl.semaphore_signal(barrier, inc=1, device_id={"tp": target(j)}, device_id_type=MESH)
    pl.semaphore_signal(barrier, inc=1, device_id={"grp": 1 - y}, device_id_type=MESH)

    @pl.when(z > 0)
    def _():
        pl.semaphore_signal(barrier, inc=1, device_id={"fs": z - 1}, device_id_type=MESH)

    @pl.when(z < n - 1)
    def _():
        pl.semaphore_signal(barrier, inc=1, device_id={"fs": z + 1}, device_id_type=MESH)

    gain_tall[...] = jnp.broadcast_to(gain_ref[...], (128, depths[0])).T

    def cast_up(j, k):
        half = depths[0] // 2
        tile = math.gcd(half, norm_tile)
        cols = wide(0, target(j))

        @pl.loop(0, half // tile)
        def _(m):
            first = pl.multiple_of(half_of(k) * half + m * tile, tile)
            here = pl.ds(first, tile)
            value = (up_stage[here, cols] * gain_tall[here, :1]).astype(jnp.bfloat16)
            if j == 0:
                up_all[pl.ds(pl.multiple_of(z * depths[0] + first, tile), tile), cols] = value
            else:
                up_cast[here, cols] = value

    def cast_down():
        tile = math.gcd(depths[1], norm_tile)

        @pl.loop(0, down_ref.shape[0] // tile)
        def _(m):
            here = pl.ds(pl.multiple_of(m * tile, tile), tile)
            down_cast[here, :] = down_stage[here, :].astype(jnp.bfloat16)

        @pl.loop(0, depths[1] // tile)
        def _(m):
            here = pl.ds(pl.multiple_of(me * depths[1] + m * tile, tile), tile)
            there = pl.ds(pl.multiple_of(z * depths[1] + m * tile, tile), tile)
            down_all[there, wide(1, me)] = down_stage[here, :].astype(jnp.bfloat16)

    def norm_rows(first, many):
        @pl.loop(0, many // norm_tile)
        def _(m):
            here = pl.ds(pl.multiple_of(first + m * norm_tile, norm_tile), norm_tile)
            values = normed[here, :].astype(jnp.float32)
            scale = lax.rsqrt(jnp.mean(values * values, axis=-1, keepdims=True) + eps)
            normed[here, :] = (values * scale).astype(jnp.bfloat16)

    def late_own(g):
        @pl.when(z == 1)
        def _():
            own_down(g).start()
            if g in doubled:
                twin_copy(g, 1, 3, 0).start()

        @pl.when(z == n - 2)
        def _():
            own_up(g).start()
            if g in doubled:
                twin_copy(g, n - 2, 3 if n > 3 else 4, n - 1).start()

    def early_own(g):
        w, j, first, _ = groups[g]
        if j > 0 and first == 0:
            tp_arrival(w, j, 0).wait_recv()

        @pl.when(z > 1)
        def _():
            own_down(g).start()

        @pl.when(z < n - 2)
        def _():
            own_up(g).start()

    def twin_own(g):
        w, j, first, _ = groups[g]
        if j > 0 and first == 0:
            tp_arrival(w, j, 1).wait_recv()
        if twins:
            for edge, near in ((0, 1), (n - 1, n - 2)):

                @pl.when(z == edge)
                def _():
                    twin_copy(g, edge, 2, near).start()

    def at_edge(body):
        for edge, way in ((0, 1), (n - 1, -1)):

            @pl.when(z == edge)
            def _():
                body(lambda s: edge + way * s)

    def edge_receive(g, a, whole=False):
        z_copy(g, a, 0, z).wait_recv()
        if not whole:
            y_copy(g, a, y).start()

    def receive_near(step):
        def edge(at):
            for g in plan[step]:
                edge_receive(g, at(1), g in doubled)

        at_edge(edge)

    def receive(step):
        @pl.when(middle)
        def _():
            for s in range(1, n - 1):
                g = step - (s - 1)
                if not 0 <= g < count:
                    continue

                @pl.when(z >= s)
                def _():
                    a = z - s
                    z_copy(g, a, 0, z).wait_recv()
                    z_copy(g, a, 0, z + 1).start()
                    if s == 1 and twins:

                        @pl.when(a != 0)
                        def _():
                            y_copy(g, a, y).start()
                    else:
                        y_copy(g, a, y).start()

                @pl.when(z + s < n)
                def _():
                    a = z + s
                    z_copy(g, a, 0, z).wait_recv()
                    z_copy(g, a, 1, z - 1).start()
                    if s == 1 and twins:

                        @pl.when(a != n - 1)
                        def _():
                            y_copy(g, a, y).start()
                    else:
                        y_copy(g, a, y).start()

        def edge(at):
            for s in range(2, n):
                g = step - (s - 2)
                if 0 <= g < count:
                    edge_receive(g, at(s))

        at_edge(edge)

    def other_half(g, a):
        y_copy(g, a, 1 - y).wait_recv()

    def other_halves(g):
        w = groups[g][0]
        half = depths[w] // 2
        ref = alls[w].at[pl.ds(0, (n - 1) * half), columns(g, source(me, groups[g][1]))]
        remote(ref, ref, half_sent(g), y_recv.at[g], {"grp": 1 - y}).wait_recv()

    tile = math.gcd(tokens, row_tile)
    step_tile = math.gcd(tokens, step_rows)

    def finish(g):
        w, j, _, width = groups[g]
        cols = columns(g, source(me, j))

        def product(a, fresh):
            deep = pl.ds(pl.multiple_of(a * depths[1], depths[1]), depths[1])

            @pl.loop(0, tokens // tile)
            def _(m):
                here = pl.ds(pl.multiple_of(m * tile, tile), tile)
                acc = jnp.dot(hidden[here, deep], down_all[deep, cols], preferred_element_type=jnp.float32)
                total[here, :] = acc if fresh else total[here, :] + acc

        if in_pieces(g):
            product(z, True)

            def partner(turn):
                return lax.rem(jnp.where(2 * z < n, z + turn, z - turn + n), n)

            @pl.loop(1, n - 1)
            def _(i):
                a = partner(i + 1)
                other_half(g, a)
                product(a, False)

            last = partner(1)
            other_half(g, last)
            deep = pl.ds(pl.multiple_of(last * depths[1], depths[1]), depths[1])

            @pl.loop(0, tokens // tile)
            def _(m):
                here = pl.ds(pl.multiple_of(m * tile, tile), tile)
                acc = jnp.dot(hidden[here, deep], down_all[deep, cols], preferred_element_type=jnp.float32)
                part[here, cols] = (total[here, :] + acc).astype(jnp.bfloat16)
        else:
            other_halves(g)

            @pl.loop(0, tokens // step_tile)
            def _(m):
                here = pl.ds(pl.multiple_of(m * step_tile, step_tile), step_tile)
                if w == 0:
                    acc = jnp.dot(normed[here, :], up_all[:, cols], preferred_element_type=jnp.float32)
                    acc = jnp.maximum(acc, 0.0)
                    hidden[here, cols] = (acc * acc).astype(jnp.bfloat16)
                else:
                    acc = jnp.dot(hidden[here, :], down_all[:, cols], preferred_element_type=jnp.float32)
                    part[here, cols] = acc.astype(jnp.bfloat16)

        if w == 1:
            for k in far_first:
                sum_copy(g, k).start()

    up_load(0).wait()
    cast_up(0, 0)
    pl.semaphore_wait(barrier, tp + (z + n - 1) // n + (2 * n - 2 - z) // n)
    for g in range(ahead):
        early_own(g)
        late_own(g)
    for j in far_first:
        up_load(j).wait()
        cast_up(j, 0)
        tp_copy(0, j, 0).start()
    late_load().wait()
    for j in far_first + [0]:
        cast_up(j, 1)
        if j > 0:
            tp_copy(0, j, 1).start()
    rows_load.wait()
    quarter = tokens // 4

    def down_work():
        down_load.wait()
        cast_down()
        for k in range(2):
            for j in far_first:
                tp_copy(1, j, k).start()

    work = [functools.partial(norm_rows, i * quarter, quarter) for i in range(4)] + [down_work]
    for g in range(ahead):
        at_edge(lambda at: edge_receive(g, at(1)))
        work.pop(0)()
    sent = ahead
    for step in range(steps):
        receive(step)
        if step < first_down + lag:
            receive_near(step)
        while sent < count and sent <= step + lead:
            early_own(sent)
            sent += 1
        for g in plan[step]:
            late_own(g)
        if step < count:
            twin_own(step)
        if work:
            work.pop(0)()
        if step >= lag:
            while work:
                work.pop(0)()
            finish(step - lag)
        if step >= first_down + lag:
            receive_near(step)

    def await_sends(ref, sem):
        remote(ref, ref, sem, sum_recv.at[0], {"grp": 1 - y}).wait_send()

    await_sends(up_cast.at[:, pl.ds(0, (tp - 1) * widths[0])], tp_send.at[0])
    await_sends(down_cast.at[pl.ds(0, (tp - 1) * depths[1]), :], tp_send.at[1])
    halves = [depth // 2 for depth in depths]
    for at in range(n):
        passed = n - 1 - (twins and at == 1) - (twins and at == n - 2)
        up_blocks = at + 1 if at < n - 1 else 0
        down_blocks = n - at if at > 0 else 0
        unequal = passed - (at in (0, n - 1))

        @pl.when(z == at)
        def _():
            if up_blocks:
                await_sends(up_all.at[pl.ds(0, up_blocks * depths[0]), :], z_send.at[0])
            if down_blocks:
                await_sends(up_all.at[pl.ds(0, down_blocks * depths[0]), :], z_send.at[1])
            if twins and at in (0, n - 1):
                await_sends(up_all.at[pl.ds(0, depths[0]), :], z_send.at[2])
            if spare and at == 1:
                await_sends(down_all.at[pl.ds(0, halves[1]), pl.ds(0, spare)], z_send.at[3])
            if spare and at == n - 2:
                way = 3 if n > 3 else 4
                await_sends(down_all.at[pl.ds(0, halves[1]), pl.ds(0, spare)], z_send.at[way])
            if passed:
                await_sends(up_all.at[pl.ds(0, passed * halves[0]), :], y_send.at[0])
                rest = pl.ds(0, model - spare)
                await_sends(down_all.at[pl.ds(0, passed * halves[1]), rest], y_send.at[1])
            if spare and unequal:
                await_sends(down_all.at[pl.ds(0, unequal * halves[1]), pl.ds(0, spare)], y_send.at[2])

    remote(arrived, arrived, sum_send.at[0], sum_recv.at[0], {"grp": 1 - y}).wait()


def place_kernel(tp, up_in, down_in, part, arrived, up_out, down_out, layer_out, layer, sem):
    share = layer.shape[0]
    me = lax.axis_index("tp")
    copies = [
        pltpu.make_async_copy(src, dst, sem.at[i])
        for i, (src, dst) in enumerate(((up_in, up_out), (down_in, down_out), (layer, layer_out)))
    ]
    copies[0].start()
    copies[1].start()

    @pl.loop(0, share // norm_tile)
    def _(m):
        here = pl.ds(pl.multiple_of(m * norm_tile, norm_tile), norm_tile)
        mine = pl.ds(pl.multiple_of(me * share + m * norm_tile, norm_tile), norm_tile)
        value = part[mine, :].astype(jnp.float32)
        for k in range(tp - 1):
            value = value + arrived[k, here, :].astype(jnp.float32)
        layer[here, :] = value.astype(jnp.bfloat16)

    copies[2].start()
    for copy in copies:
        copy.wait()


def on_device(prompt_rows, up_master, down_master, norm_gain):
    n = lax.axis_size("fs")
    tp = lax.axis_size("tp")
    bf16 = jnp.bfloat16
    up_rows, width = up_master.shape
    span = width // n
    fs_per_tp = n // tp
    up_width = fs_per_tp * span
    down_width = down_master.shape[1]
    if fs_per_tp > 1:
        up_master = up_master.reshape(up_rows, fs_per_tp, tp, span).swapaxes(1, 2)
        up_master = up_master.reshape(up_rows, width)
    groups = column_groups(tp, (up_width, down_width))
    count = len(groups)
    tokens, model = prompt_rows.shape
    units = n * span
    share = tokens // tp
    vmem = pl.BlockSpec(memory_space=pltpu.VMEM)
    hbm = pl.BlockSpec(memory_space=pl.ANY)
    dma = pltpu.SemaphoreType.DMA
    held = pl.pallas_call(
        functools.partial(gather_kernel, n, tp, groups),
        out_shape=(
            pltpu.VMEM((model, units), bf16),
            pltpu.VMEM((units, model), bf16),
            pltpu.VMEM((tokens, model), bf16),
            pltpu.VMEM((tp - 1, share, model), bf16),
        ),
        in_specs=[hbm, hbm, vmem, hbm],
        out_specs=(vmem, vmem, vmem, vmem),
        scratch_shapes=[
            pltpu.VMEM((tokens, model), bf16),
            pltpu.VMEM((tokens, units), bf16),
            pltpu.VMEM((tokens, groups[-1][3]), jnp.float32),
            pltpu.VMEM(up_master.shape, jnp.float32),
            pltpu.VMEM(down_master.shape, jnp.float32),
            pltpu.VMEM(up_master.shape, bf16),
            pltpu.VMEM(down_master.shape, bf16),
            pltpu.VMEM((up_rows, 128), jnp.float32),
            dma((tp + 3,)),
            dma((2,)),
            dma((2, tp - 1, 2)),
            dma((5,)),
            dma((count, n - 1)),
            dma((3,)),
            dma((count + pieces * n,)),
            dma((1,)),
            dma((1,)),
        ],
        compiler_params=pltpu.CompilerParams(
            collective_id=0, has_side_effects=True, vmem_limit_bytes=32 * 1024 * 1024
        ),
    )(up_master, down_master, norm_gain[None, :], prompt_rows)
    up_sampler, down_sampler, layer_out = pl.pallas_call(
        functools.partial(place_kernel, tp),
        out_shape=(
            jax.ShapeDtypeStruct((model, units), bf16),
            jax.ShapeDtypeStruct((units, model), bf16),
            jax.ShapeDtypeStruct((share, model), bf16),
        ),
        in_specs=[vmem] * 4,
        out_specs=(hbm, hbm, hbm),
        scratch_shapes=[pltpu.VMEM((share, model), bf16), dma((3,))],
        compiler_params=pltpu.CompilerParams(vmem_limit_bytes=8 * 1024 * 1024),
    )(*held)
    return (up_sampler[None], down_sampler[None], layer_out)


def solution(mesh):
    in_specs = (P(("grp", "fs"), None), P("fs", "tp"), P("fs", "tp"), P("fs"))
    out_specs = (
        P(("grp", "tp"), None, None),
        P(("grp", "tp"), None, None),
        P(("grp", "fs", "tp"), None),
    )
    return jax.shard_map(
        on_device, mesh=mesh, in_specs=in_specs, out_specs=out_specs, check_vma=False
    )
```
